32 devices in a mesh: sp: 8 (over z, y), dp: 4 (over x, core).
Axes of the slice: x: 2, y: 2, z: 4, core: 2. Of those that a mesh axis runs over, the one named last changes fastest.
Arguments:
- queries: bfloat16 [4, 1024, 16, 128], P('dp', 'sp'), may hold values from -7 to 7
- key_vectors: bfloat16 [4, 1024, 16, 128], P('dp', 'sp'), may hold values from -6 to 6
- value_vectors: bfloat16 [4, 1024, 16, 128], P('dp', 'sp'), may hold values from -6 to 6
- head_lambda: float32 [16], P('sp'), may hold values from 0.3 to 0.8
- head_gain: float32 [128], replicated, may hold values from 0.1 to 1.9
- residual: bfloat16 [4, 1024, 2048], P('dp', 'sp'), may hold values from -6 to 6
- out_weight: bfloat16 [2048, 2048], replicated, may hold values from -0.125 to 0.125
- mix_gain: float32 [2048], replicated, may hold values from 0.1 to 1.9
- pre_gain: float32 [2048], replicated, may hold values from 0.1 to 1.9
- post_gain: float32 [2048], replicated, may hold values from 0.1 to 1.9
- routes: int32 [4, 1024, 4], P('dp', 'sp'), may hold values from 0 to 31, all different within a row; in each aligned block of 128 rows (0 to 127, 128 to 255, ..., all dimensions but the last counted through in order) at most 24 rows name the same one
- route_weights: float32 [4, 1024, 4], P('dp', 'sp'), may hold values from 0.25 to 1
- expert_gate: bfloat16 [32, 2048, 512], P(('sp', 'dp')), may hold values from -0.125 to 0.125
- expert_up: bfloat16 [32, 2048, 512], P(('sp', 'dp')), may hold values from -0.125 to 0.125
- expert_down: bfloat16 [32, 512, 2048], P(('sp', 'dp')), may hold values from -0.25 to 0.25
- shared_gate: bfloat16 [2048, 512], replicated, may hold values from -0.125 to 0.125
- shared_up: bfloat16 [2048, 512], replicated, may hold values from -0.125 to 0.125
- shared_down: bfloat16 [512, 2048], replicated, may hold values from -0.25 to 0.25
Outputs:
- output: bfloat16 [4, 1024, 2048], P('dp', 'sp')
The draws below stay inside these ranges and needn't reach their ends.
Inputs may be any that keep to these rules, and one draw needn't show every extreme that they name: `routes`: among the tokens of one device (aligned blocks of 128 positions), no expert is named more than 24 times; in some block some expert is named exactly 24 times. Each token names 4 different experts.
All inputs are finite; a program needn't handle non-finite values.
Results may differ from the reference program's by a relative error of at most 0.0075.
Values may be sent and summed in bfloat16 or wider, within the bound.
No kernel may reach another device: no remote copies, remote signals or barrier semaphores. Data moves between devices by JAX's collectives and lax.ppermute only.
A program may use at most 128 MiB of HBM per device.

```python
import math
import jax
import jax.numpy as jnp
import numpy as np
from jax import lax

D = 2048
HEADS = 16
HD = 64
VD = 128
FF = 512
TOP_K = 4
TOK_DEV = 128
LEN = 1024
SEQS = 4
EXPERTS = 32
CAP = 24


def draw_queries(key, part):
    shape = (SEQS, LEN, HEADS, 2 * HD)
    base_key = jax.random.fold_in(key, 11)
    drawn = jnp.clip(1.75 * jax.random.normal(base_key, shape, jnp.float32), -7.0, 7.0)
    return drawn.astype(jnp.bfloat16)


def draw_key_vectors(key, part):
    shape = (SEQS, LEN, HEADS, 2 * HD)
    base_key = jax.random.fold_in(key, 13)
    drawn = jnp.clip(jax.random.normal(base_key, shape, jnp.float32), -6.0, 6.0)
    return drawn.astype(jnp.bfloat16)


def levels(key, dims, cuts, least, top_value):
    def one(position, parts):
        draws = jax.random.uniform(jax.random.fold_in(jax.random.fold_in(key, 6), position), (parts,), jnp.float32, least / len(cuts), top_value / len(cuts))
        return jnp.repeat(jnp.exp(draws), dims[position] // parts).reshape((-1,) + (1,) * (len(dims) - position - 1))

    level = one(*cuts[0])
    for cut in cuts[1:]:
        level = level * one(*cut)
    return level


def deal_out(rng, own, number, rows, amount, top, reach, slope):
    sequence = jax.random.permutation(rng, amount)
    heavy_load, common = portions_of(amount, rows * top, reach, slope, True), portions_of(amount, rows * top, reach, slope, False)
    places = jnp.arange(amount)

    def named(lengths, rotation):
        used = int((lengths > 0).sum())
        fixed = max(1, used // 4)
        passed = fixed + (places - fixed + rotation * (used - fixed)) % max(1, amount - fixed)
        return jnp.zeros((amount,), jnp.int32).at[sequence[jnp.where(places < fixed, places, passed)]].set(jnp.asarray(lengths, jnp.int32))

    lengths = jnp.where(number % 4 == 0, named(heavy_load, number // 4), named(common, number - number // 4 - 1))
    mixed = jax.random.permutation(jax.random.fold_in(own, 3), amount)
    source_of, sink = mixed[0:amount // 2 * 2:2], mixed[1:amount // 2 * 2:2]
    room = jnp.minimum(lengths[source_of] - 1, reach - lengths[sink]) // 2
    room = jnp.where((source_of == sequence[0]) | (sink == sequence[0]) | (lengths[sink] == 0), 0, jnp.maximum(room, 0))
    passed = jax.random.randint(jax.random.fold_in(own, 4), (amount // 2,), 0, 1 << 20) % (room + 1)
    lengths = lengths.at[source_of].add(-passed).at[sink].add(passed)
    members = jnp.searchsorted(jnp.cumsum(lengths), jnp.arange(rows * top), side="right").astype(jnp.int32)
    listing = members.reshape(top, rows).T
    listing = listing[jax.random.permutation(jax.random.fold_in(own, 1), rows)]
    rotation = jax.random.randint(jax.random.fold_in(own, 2), (rows, 1), 0, top)
    return jnp.take_along_axis(listing, (jnp.arange(top)[None, :] + rotation) % top, axis=1)


def portions_of(count, total, reach, lean, full):
    weights = [(1 << 20) // math.isqrt(grade ** lean) + 1 for grade in range(1, count + 1)]
    largest = reach if full else min(reach, max(-(-total // count), total * weights[0] // sum(weights)))
    least = 1 if total - largest >= count - 1 else 0
    counts, spare = [largest] + [least] * (count - 1), total - largest - least * (count - 1)
    while spare > 0:
        candidates = [i for i in range(1, count) if counts[i] < largest] or [i for i in range(1, count) if counts[i] < reach]
        whole, remaining = sum([weights[i] for i in candidates]), spare
        for i in candidates:
            extra = min(reach - counts[i], max(1, remaining * weights[i] // whole), spare)
            counts[i] = counts[i] + extra
            spare = spare - extra
    return np.array(counts)


def bell_draw(rng, dims, spread, reach, pieces=(), held_as=jnp.bfloat16):
    values = spread * jax.random.normal(rng, dims, jnp.float32)
    if pieces:
        values = values * levels(rng, dims, pieces, -0.22, 0.18)
    return jnp.clip(values, -reach, reach).astype(held_as)


def setup_inputs(seed: int = 0) -> dict:
    key_list = jax.random.split(jax.random.key(seed), 19)
    queries = draw_queries(jax.random.fold_in(key_list[18], 71), 0)
    key_vectors = draw_key_vectors(jax.random.fold_in(key_list[18], 71), 0)
    value_vectors = bell_draw(key_list[2], (SEQS, LEN, HEADS, VD), 1.0, 6.0, ((0, 4), (1, 8)))
    head_lambda = jnp.clip(0.3 + 0.5 * jax.random.uniform(key_list[3], (HEADS,), jnp.float32) ** levels(key_list[3], (HEADS,), ((0, 8),), -0.2, 0.2), 0.3, 0.8)
    head_gain = jnp.clip(1.0 + 0.18 * jax.random.normal(key_list[4], (VD,), jnp.float32), 0.1, 1.9)
    residual = bell_draw(key_list[5], (SEQS, LEN, D), 1.0, 6.0, ((0, 4), (1, 8)))
    out_weight = bell_draw(key_list[6], (HEADS * VD, D), (HEADS * VD) ** -0.5, 0.125)
    mix_gain = jnp.clip(1.0 + 0.18 * jax.random.normal(key_list[7], (D,), jnp.float32), 0.1, 1.9)
    pre_gain = jnp.clip(1.0 + 0.18 * jax.random.normal(key_list[8], (D,), jnp.float32), 0.1, 1.9)
    post_gain = jnp.clip(1.0 + 0.18 * jax.random.normal(key_list[9], (D,), jnp.float32), 0.1, 1.9)
    routes_keys = jax.random.split(jax.random.fold_in(key_list[10], 1), SEQS * LEN // TOK_DEV)
    routes_turns = jax.random.permutation(jax.random.fold_in(key_list[10], 3), SEQS * LEN // TOK_DEV)
    routes = jax.vmap(lambda own, number: deal_out(jax.random.fold_in(key_list[10], 2), own, number, TOK_DEV, EXPERTS, TOP_K, CAP, 2))(routes_keys, routes_turns).reshape((SEQS, LEN, TOP_K))
    route_weights = jnp.clip(0.25 + 0.75 * jax.random.uniform(key_list[11], (SEQS, LEN, TOP_K), jnp.float32) ** levels(key_list[11], (SEQS, LEN, TOP_K), ((0, 4), (1, 8)), -0.2, 0.2), 0.25, 1.0)
    expert_gate = bell_draw(key_list[12], (EXPERTS, D, FF), D ** -0.5, 0.125, ((0, 32),))
    expert_up = bell_draw(key_list[13], (EXPERTS, D, FF), D ** -0.5, 0.125, ((0, 32),))
    expert_down = bell_draw(key_list[14], (EXPERTS, FF, D), FF ** -0.5, 0.25, ((0, 32),))
    shared_gate = bell_draw(key_list[15], (D, FF), D ** -0.5, 0.125)
    shared_up = bell_draw(key_list[16], (D, FF), D ** -0.5, 0.125)
    shared_down = bell_draw(key_list[17], (FF, D), FF ** -0.5, 0.25)
    return dict(queries=queries, key_vectors=key_vectors, value_vectors=value_vectors, head_lambda=head_lambda, head_gain=head_gain, residual=residual, out_weight=out_weight, mix_gain=mix_gain, pre_gain=pre_gain, post_gain=post_gain, routes=routes, route_weights=route_weights, expert_gate=expert_gate, expert_up=expert_up, expert_down=expert_down, shared_gate=shared_gate, shared_up=shared_up, shared_down=shared_down)


epsilon = 1e-06

def rms_scale(values_in, gain):
    return values_in * lax.rsqrt(lax.optimization_barrier(jnp.mean(values_in * values_in, axis=-1, keepdims=True)) + epsilon) * gain

def feed_forward(rows, gate_w, up_w, down_w):
    gate_val = jnp.dot(rows, gate_w, preferred_element_type=jnp.float32)
    up_val = jnp.dot(rows, up_w, preferred_element_type=jnp.float32)
    hidden = (jax.nn.silu(gate_val) * up_val).astype(jnp.bfloat16)
    return jnp.dot(hidden, down_w, preferred_element_type=jnp.float32).astype(jnp.bfloat16)

def attend_sequence(query_seq, key_seq, value_seq, head_lambda, head_gain):
    length = query_seq.shape[0]
    head_count = query_seq.shape[1]
    head_size = query_seq.shape[2] // 2
    block_rows = min(512, length)
    block_count = length // block_rows
    query_blocks = query_seq.astype(jnp.float32).reshape(block_count, block_rows, head_count, 2, head_size)
    key_all = key_seq.astype(jnp.float32).reshape(length, head_count, 2, head_size)
    value_all = value_seq.astype(jnp.float32)
    key_pos = jnp.arange(length, dtype=jnp.int32)

    def one_block(inputs):
        query_block, block_index = inputs
        scores = jnp.einsum('qhmd,khmd->hmqk', query_block, key_all) * head_size ** (-0.5)
        query_pos = block_index * block_rows + jnp.arange(block_rows, dtype=jnp.int32)
        causal = key_pos[None, :] <= query_pos[:, None]
        scores = jnp.where(causal, scores, -jnp.inf)
        maxima = lax.optimization_barrier(jnp.max(scores, axis=-1, keepdims=True))
        exponent = jnp.exp(scores - maxima)
        softmax_both = exponent / lax.optimization_barrier(jnp.sum(exponent, axis=-1, keepdims=True))
        mixture = softmax_both[:, 0] - head_lambda[:, None, None] * softmax_both[:, 1]
        mixture_low = lax.optimization_barrier(mixture.astype(jnp.bfloat16)).astype(jnp.float32)
        head_output = jnp.einsum('hqk,khe->qhe', mixture_low, value_all)
        return rms_scale(head_output, head_gain).astype(jnp.bfloat16)
    outputs = lax.map(one_block, (query_blocks, jnp.arange(block_count, dtype=jnp.int32)))
    return outputs.reshape(length, head_count, -1)

def reference(queries, key_vectors, value_vectors, head_lambda, head_gain, residual, out_weight, mix_gain, pre_gain, post_gain, routes, route_weights, expert_gate, expert_up, expert_down, shared_gate, shared_up, shared_down):
    heads_out = lax.map(lambda inputs: attend_sequence(inputs[0], inputs[1], inputs[2], head_lambda, head_gain), (queries, key_vectors, value_vectors))
    token_total = SEQS * LEN
    flat_heads = heads_out.reshape(token_total, HEADS * VD)
    mixed_rows = jnp.dot(flat_heads, out_weight, preferred_element_type=jnp.float32)
    updated = (residual.reshape(token_total, D).astype(jnp.float32) + rms_scale(mixed_rows, mix_gain)).astype(jnp.bfloat16)
    normed = rms_scale(updated.astype(jnp.float32), pre_gain).astype(jnp.bfloat16)
    shared_out = feed_forward(normed, shared_gate, shared_up, shared_down)
    block_total = token_total // TOK_DEV
    assign_block = TOK_DEV * TOP_K
    flat_routes = routes.reshape(block_total, assign_block).astype(jnp.int32)
    one_hot = (flat_routes[:, :, None] == jnp.arange(EXPERTS, dtype=jnp.int32)[None, None, :]).astype(jnp.int32)
    earlier = jnp.cumsum(one_hot, axis=1) - one_hot
    rank_index = lax.optimization_barrier(jnp.sum(earlier * one_hot, axis=2))
    block_ids = jnp.arange(block_total, dtype=jnp.int32)[:, None]
    slot_index = (flat_routes * (block_total * CAP) + block_ids * CAP + rank_index).reshape(-1)
    assign_ids = jnp.arange(block_total * assign_block, dtype=jnp.int32)
    source_table = jnp.zeros((EXPERTS * block_total * CAP,), jnp.int32).at[slot_index].set(assign_ids)
    rows_per_expert = source_table.reshape(EXPERTS, block_total * CAP) // TOP_K

    def run_expert(inputs):
        row_ids, gate_w, up_w, down_w = inputs
        return feed_forward(normed[row_ids], gate_w, up_w, down_w)
    expert_out = lax.map(run_expert, (rows_per_expert, expert_gate, expert_up, expert_down))
    picked = expert_out.reshape(EXPERTS * block_total * CAP, D)[slot_index]
    routed = lax.optimization_barrier(jnp.sum(picked.astype(jnp.float32).reshape(token_total, TOP_K, D) * route_weights.reshape(token_total, TOP_K, 1), axis=1))
    combined = routed + shared_out.astype(jnp.float32)
    output = (updated.astype(jnp.float32) + rms_scale(combined, post_gain)).astype(jnp.bfloat16)
    return output.reshape(SEQS, LEN, D)
```

```python
import jax
import jax.numpy as jnp
from jax import lax
from jax.experimental import pallas as pl
from jax.experimental.pallas import tpu as pltpu
from jax.sharding import PartitionSpec as P

epsilon = 1e-06


def rms_scale(values_in, gain):
    return (
        values_in
        * lax.rsqrt(jnp.mean(values_in * values_in, axis=-1, keepdims=True) + epsilon)
        * gain
    )


def feed_forward(rows, gate_w, up_w, down_w):
    gate_val = jnp.dot(rows, gate_w, preferred_element_type=jnp.float32)
    up_val = jnp.dot(rows, up_w, preferred_element_type=jnp.float32)
    hidden = (jax.nn.silu(gate_val) * up_val).astype(jnp.bfloat16)
    return jnp.dot(hidden, down_w, preferred_element_type=jnp.float32).astype(jnp.bfloat16)


def attend(packed, head_lambda, head_gain):
    length = packed.shape[0]
    head_count = head_lambda.shape[0]
    width = head_gain.shape[0]
    half = width // 2
    block = min(256, length)
    scale = half ** (-0.5)

    def body(lambda_ref, packed_ref, gain_ref, out_ref):
        lane = lax.broadcasted_iota(jnp.int32, (block, width), 1)
        row = lax.broadcasted_iota(jnp.int32, (block, block), 0)
        col = lax.broadcasted_iota(jnp.int32, (block, block), 1)
        causal = col <= row
        gain = gain_ref[...]
        contract = (((1,), (1,)), ((), ()))
        for head in range(head_count):
            q_col, k_col, v_col = (
                (part * head_count + head) * width for part in range(3)
            )
            for index in range(length // block):
                start = index * block
                query = packed_ref[start : start + block, q_col : q_col + width]
                query = query.astype(jnp.float32) * scale
                spans = ([(0, start)] if index else []) + [(start, start + block)]
                weights = []
                for part in range(2):
                    keep = (lane < half) if part == 0 else (lane >= half)
                    one = jnp.where(keep, query, 0.0).astype(jnp.bfloat16)
                    scores = [
                        lax.dot_general(
                            one,
                            packed_ref[low:high, k_col : k_col + width],
                            contract,
                            preferred_element_type=jnp.float32,
                        )
                        for low, high in spans
                    ]
                    scores[-1] = jnp.where(causal, scores[-1], -jnp.inf)
                    top = scores[0].max(axis=1, keepdims=True)
                    for other in scores[1:]:
                        top = jnp.maximum(top, other.max(axis=1, keepdims=True))
                    powers = [jnp.exp(s - top) for s in scores]
                    total = powers[0].sum(axis=1, keepdims=True)
                    for other in powers[1:]:
                        total = total + other.sum(axis=1, keepdims=True)
                    factor = 1.0 / total
                    if part == 1:
                        factor = factor * lambda_ref[head]
                    weights.append((powers, factor))
                result = None
                for place, (low, high) in enumerate(spans):
                    mixture = (
                        weights[0][0][place] * weights[0][1]
                        - weights[1][0][place] * weights[1][1]
                    ).astype(jnp.bfloat16)
                    piece = jnp.dot(
                        mixture,
                        packed_ref[low:high, v_col : v_col + width],
                        preferred_element_type=jnp.float32,
                    )
                    result = piece if result is None else result + piece
                out_ref[start : start + block, head * width : (head + 1) * width] = rms_scale(
                    result, gain
                ).astype(jnp.bfloat16)

    return pl.pallas_call(
        body,
        out_shape=jax.ShapeDtypeStruct((length, head_count * width), jnp.bfloat16),
        in_specs=[
            pl.BlockSpec(memory_space=pltpu.SMEM),
            pl.BlockSpec(memory_space=pltpu.VMEM),
            pl.BlockSpec(memory_space=pltpu.VMEM),
        ],
        out_specs=pl.BlockSpec(memory_space=pltpu.VMEM),
        compiler_params=pltpu.CompilerParams(vmem_limit_bytes=48 * 1024 * 1024),
        name="attend",
    )(head_lambda, packed, head_gain.reshape(1, width))


def finish(returned, high, low, shared_out, updated, post_gain):
    def body(ret_ref, high_ref, low_ref, shared_ref, updated_ref, gain_ref, out_ref):
        rows = ret_ref[...]
        combined = (
            jnp.dot(high_ref[...], rows, preferred_element_type=jnp.float32)
            + jnp.dot(low_ref[...], rows, preferred_element_type=jnp.float32)
            + shared_ref[...].astype(jnp.float32)
        )
        out_ref[...] = (
            updated_ref[...].astype(jnp.float32) + rms_scale(combined, gain_ref[...])
        ).astype(jnp.bfloat16)

    return pl.pallas_call(
        body,
        out_shape=jax.ShapeDtypeStruct(updated.shape, jnp.bfloat16),
        in_specs=[pl.BlockSpec(memory_space=pltpu.VMEM)] * 6,
        out_specs=pl.BlockSpec(memory_space=pltpu.VMEM),
        compiler_params=pltpu.CompilerParams(vmem_limit_bytes=48 * 1024 * 1024),
        name="finish",
    )(returned, high, low, shared_out, updated, post_gain.reshape(1, -1))


def slots_of(routes, experts_total, capacity):
    tok_count = routes.shape[0]
    expert_ids = jnp.arange(experts_total, dtype=jnp.int32)
    chosen = routes[:, :, None] == expert_ids[None, None, :]
    named = jnp.any(chosen, axis=1).astype(jnp.bfloat16)
    token_ids = jnp.arange(tok_count, dtype=jnp.int32)
    before = (token_ids[None, :] < token_ids[:, None]).astype(jnp.bfloat16)
    rank = jnp.dot(before, named, preferred_element_type=jnp.float32)
    own_rank = jnp.sum(jnp.where(chosen, rank[:, None, :], 0.0), axis=2).astype(jnp.int32)
    return routes * capacity + own_rank


def local(
    queries,
    key_vectors,
    value_vectors,
    head_lambda,
    head_gain,
    residual,
    out_weight,
    mix_gain,
    pre_gain,
    post_gain,
    routes,
    route_weights,
    expert_gate,
    expert_up,
    expert_down,
    shared_gate,
    shared_up,
    shared_down,
):
    sp_size = lax.axis_size("sp")
    tok_count, heads_total, width = queries.shape[1:]
    head_count = heads_total // sp_size
    packed = jnp.concatenate(
        [
            jnp.transpose(
                part[0].reshape(tok_count, sp_size, head_count * width), (1, 0, 2)
            )
            for part in (queries, key_vectors, value_vectors)
        ],
        axis=2,
    )
    packed = lax.all_to_all(packed, "sp", split_axis=0, concat_axis=0, tiled=True)
    attended = attend(
        packed.reshape(sp_size * tok_count, 3 * head_count * width), head_lambda, head_gain
    )
    token_heads = lax.all_to_all(
        attended.reshape(sp_size, tok_count, head_count * width),
        "sp",
        split_axis=0,
        concat_axis=0,
        tiled=True,
    )

    experts_total = sp_size * lax.axis_size("dp")
    top_count = routes.shape[2]
    capacity = 3 * tok_count * top_count // (2 * experts_total)
    slot_total = experts_total * capacity
    slots = slots_of(routes[0], experts_total, capacity)
    slot_ids = jnp.arange(slot_total, dtype=jnp.int32)
    pick = slots[:, :, None] == slot_ids[None, None, :]
    weight_rows = jnp.sum(jnp.where(pick, route_weights[0][:, :, None], 0.0), axis=1)
    high_part = lax.reduce_precision(weight_rows, 8, 7)
    high = high_part.astype(jnp.bfloat16)
    low = (weight_rows - high_part).astype(jnp.bfloat16)
    slots_t = slots.T
    place = (slots_t[0][None, :] == slot_ids[:, None]).astype(jnp.bfloat16)
    for k in range(1, top_count):
        place = place + (slots_t[k][None, :] == slot_ids[:, None]).astype(jnp.bfloat16)

    flat_heads = jnp.transpose(token_heads, (1, 0, 2)).reshape(tok_count, -1)
    mixed_rows = jnp.dot(flat_heads, out_weight, preferred_element_type=jnp.float32)
    updated = (residual[0].astype(jnp.float32) + rms_scale(mixed_rows, mix_gain)).astype(
        jnp.bfloat16
    )
    normed = rms_scale(updated.astype(jnp.float32), pre_gain).astype(jnp.bfloat16)
    model_width = normed.shape[1]
    outgoing = jnp.dot(place, normed, preferred_element_type=jnp.float32).astype(jnp.bfloat16)
    outgoing = outgoing.reshape(experts_total, capacity, model_width)
    arrived = lax.all_to_all(outgoing, ("sp", "dp"), split_axis=0, concat_axis=0, tiled=True)
    shared_out = feed_forward(normed, shared_gate, shared_up, shared_down)
    flat_rows = arrived.reshape(-1, model_width)
    result_rows = feed_forward(flat_rows, expert_gate[0], expert_up[0], expert_down[0])
    results = result_rows.reshape(arrived.shape[0], -1, model_width)
    returned = lax.all_to_all(results, ("sp", "dp"), split_axis=0, concat_axis=0, tiled=True)
    output = finish(
        returned.reshape(slot_total, model_width), high, low, shared_out, updated, post_gain
    )
    return output.reshape(1, tok_count, model_width)


def solution(mesh):
    in_specs = (
        P("dp", "sp", None, None),
        P("dp", "sp", None, None),
        P("dp", "sp", None, None),
        P("sp"),
        P(),
        P("dp", "sp", None),
        P(),
        P(),
        P(),
        P(),
        P("dp", "sp", None),
        P("dp", "sp", None),
        P(("sp", "dp"), None, None),
        P(("sp", "dp"), None, None),
        P(("sp", "dp"), None, None),
        P(),
        P(),
        P(),
    )
    out_specs = P("dp", "sp", None)
    return jax.shard_map(local, mesh=mesh, in_specs=in_specs, out_specs=out_specs, check_vma=False)
```
